256 devices in a mesh: ep: 64 (over z, x, core), tp: 4 (over y).
Axes of the slice: x: 4, y: 4, z: 8, core: 2. Of those that a mesh axis runs over, the one named last changes fastest.
Arguments:
- queries: bfloat16 [16384, 2, 1024], P('ep', None, 'tp')
- keys: bfloat16 [16384, 2, 256], P('ep', None, 'tp')
- values: bfloat16 [16384, 2, 256], P('ep', None, 'tp'), may hold values from -6 to 6
- query_gain: float32 [64], replicated, may hold values from 1.2 to 6
- key_gain: float32 [64], replicated, may hold values from 1.2 to 6
- out_weight: bfloat16 [1024, 2048], P('tp'), may hold values from -0.75 to 0.75
- moe_tokens: bfloat16 [32768, 2048], P(('ep', 'tp')), may hold values from -6 to 6
- moe_gain: float32 [2048], replicated, may hold values from 0.1 to 1.9
- routes: int32 [32768, 2], P(('ep', 'tp')), may hold values from 0 to 63, all different within a row; in each aligned block of 128 rows (0 to 127, 128 to 255, ...) at most 6 rows name the same one
- route_weight: float32 [32768, 2], P(('ep', 'tp')), may hold values from 0.1 to 1
- w_gate: bfloat16 [64, 2048, 1024], P('ep', None, 'tp'), may hold values from -0.125 to 0.125
- w_up: bfloat16 [64, 2048, 1024], P('ep', None, 'tp'), may hold values from -0.125 to 0.125
- w_down: bfloat16 [64, 1024, 2048], P('ep', 'tp'), may hold values from -0.1875 to 0.1875
Outputs:
- attended: bfloat16 [16384, 2, 2048], P(('ep', 'tp'))
- routed: bfloat16 [32768, 2048], P(('ep', 'tp'))
The draws below stay inside these ranges and needn't reach their ends.
Inputs may be any that keep to these rules, and one draw needn't show every extreme that they name: `routes`: each row names 2 different experts. The rows of one device name no expert more than 6 times, and in every draw some device's rows name one expert exactly 6 times.
All inputs are finite; a program needn't handle non-finite values.
Results may differ from the reference program's by a relative error of at most 0.013.
The reference program's roundings to bfloat16 on the way count: a program that leaves them out, or rounds other values in their place, can miss the bound.
Values may be sent and summed in bfloat16 or wider, within the bound.
A program may use at most 128 MiB of HBM per device.

```python
import math
import jax
import jax.numpy as jnp
import numpy as np
from jax import lax

D = 2048
HEADS = 16
KV_HEADS = 4
HEAD_DIM = 64
FF = 1024
TOPK = 2
GRID_W = 64
SEQS = 2
TOK_DEV = 128
LEN = 16384
EXPERTS = 64
CAP = 6
TOKENS = 32768
N_EP = 64
N_TP = 4


def draw_both(key):
    keys_drawn = jax.random.normal(jax.random.fold_in(key, 12), (LEN, SEQS, KV_HEADS * HEAD_DIM), jnp.float32)
    queries_drawn = jax.random.normal(jax.random.fold_in(key, 11), (LEN, SEQS, HEADS * HEAD_DIM), jnp.float32)
    return (queries_drawn, keys_drawn)


def draw_queries(key, part):
    return draw_both(key)[0].astype(jnp.bfloat16)


def draw_keys(key, part):
    return draw_both(key)[1].astype(jnp.bfloat16)


def draw_gain_values(key):
    return jax.random.uniform(key, (HEAD_DIM,), jnp.float32, 1.2, 2.0)


def draw_query_gain(key, part):
    return draw_gain_values(jax.random.fold_in(key, 21))


def draw_key_gain(key, part):
    return draw_gain_values(jax.random.fold_in(key, 22))


def shard_levels(own_key, shape, split, least, high):
    def one(position, blocks):
        draws = jax.random.uniform(jax.random.fold_in(jax.random.fold_in(own_key, 6), position), (blocks,), jnp.float32, least / len(split), high / len(split))
        return jnp.repeat(jnp.exp(draws), shape[position] // blocks).reshape((-1,) + (1,) * (len(shape) - position - 1))

    level = one(*split[0])
    for cut in split[1:]:
        level = level * one(*cut)
    return level


def shared_out(key, own, number, rows, count, top, limit, skew):
    order = jax.random.permutation(key, count)
    heavy_load, common = load_shares(count, rows * top, limit, skew, True), load_shares(count, rows * top, limit, skew, False)
    places = jnp.arange(count)

    def named(sizes, turn):
        used = int((sizes > 0).sum())
        fixed = max(1, used // 4)
        passed = fixed + (places - fixed + turn * (used - fixed)) % max(1, count - fixed)
        return jnp.zeros((count,), jnp.int32).at[order[jnp.where(places < fixed, places, passed)]].set(jnp.asarray(sizes, jnp.int32))

    sizes = jnp.where(number % 4 == 0, named(heavy_load, number // 4), named(common, number - number // 4 - 1))
    mixed = jax.random.permutation(jax.random.fold_in(own, 3), count)
    source_of, sink = mixed[0:count // 2 * 2:2], mixed[1:count // 2 * 2:2]
    margin = jnp.minimum(sizes[source_of] - 1, limit - sizes[sink]) // 2
    margin = jnp.where((source_of == order[0]) | (sink == order[0]) | (sizes[sink] == 0), 0, jnp.maximum(margin, 0))
    passed = jax.random.randint(jax.random.fold_in(own, 4), (count // 2,), 0, 1 << 20) % (margin + 1)
    sizes = sizes.at[source_of].add(-passed).at[sink].add(passed)
    members = jnp.searchsorted(jnp.cumsum(sizes), jnp.arange(rows * top), side="right").astype(jnp.int32)
    table = members.reshape(top, rows).T
    table = table[jax.random.permutation(jax.random.fold_in(own, 1), rows)]
    turn = jax.random.randint(jax.random.fold_in(own, 2), (rows, 1), 0, top)
    return jnp.take_along_axis(table, (jnp.arange(top)[None, :] + turn) % top, axis=1)


def load_shares(number_of, total, most, slope, full):
    weights = [(1 << 20) // math.isqrt(standing ** slope) + 1 for standing in range(1, number_of + 1)]
    largest = most if full else min(most, max(-(-total // number_of), total * weights[0] // sum(weights)))
    least = 1 if total - largest >= number_of - 1 else 0
    counts, spare = [largest] + [least] * (number_of - 1), total - largest - least * (number_of - 1)
    while spare > 0:
        movable = [i for i in range(1, number_of) if counts[i] < largest] or [i for i in range(1, number_of) if counts[i] < most]
        whole, budget = sum([weights[i] for i in movable]), spare
        for i in movable:
            addition = min(most - counts[i], max(1, budget * weights[i] // whole), spare)
            counts[i] = counts[i] + addition
            spare = spare - addition
    return np.array(counts)


def normal_values(rng, shape, scale, limit, cuts=(), held_as=jnp.bfloat16):
    result = scale * jax.random.normal(rng, shape, jnp.float32)
    if cuts:
        result = result * shard_levels(rng, shape, cuts, -0.22, 0.18)
    return jnp.clip(result, -limit, limit).astype(held_as)


def setup_inputs(seed: int = 0) -> dict:
    seeds = jax.random.split(jax.random.key(seed), 14)
    queries = draw_queries(jax.random.fold_in(seeds[13], 71), 0)
    keys = draw_keys(jax.random.fold_in(seeds[13], 71), 0)
    values = normal_values(seeds[2], (LEN, SEQS, KV_HEADS * HEAD_DIM), 1.0, 6.0, ((0, 64), (2, 4)))
    query_gain = draw_query_gain(jax.random.fold_in(seeds[13], 71), 0)
    key_gain = draw_key_gain(jax.random.fold_in(seeds[13], 71), 0)
    out_weight = normal_values(seeds[5], (HEADS * HEAD_DIM, D), (HEADS * HEAD_DIM // 16) ** -0.5, 0.75, ((0, 4),))
    moe_tokens = normal_values(seeds[6], (TOKENS, D), 1.0, 6.0, ((0, 256),))
    moe_gain = jnp.clip(1.0 + 0.18 * jax.random.normal(seeds[7], (D,), jnp.float32), 0.1, 1.9)
    routes_keys = jax.random.split(jax.random.fold_in(seeds[8], 1), TOKENS // TOK_DEV)
    routes_turns = jax.random.permutation(jax.random.fold_in(seeds[8], 3), TOKENS // TOK_DEV)
    routes = jax.vmap(lambda own, number: shared_out(jax.random.fold_in(seeds[8], 2), own, number, TOK_DEV, EXPERTS, TOPK, CAP, 1))(routes_keys, routes_turns).reshape((TOKENS, TOPK))
    route_weight = jnp.clip(0.1 + 0.9 * jax.random.uniform(seeds[9], (TOKENS, TOPK), jnp.float32) ** shard_levels(seeds[9], (TOKENS, TOPK), ((0, 256),), -0.2, 0.2), 0.1, 1.0)
    w_gate = normal_values(seeds[10], (EXPERTS, D, FF), D ** -0.5, 0.125, ((0, 64), (2, 4)))
    w_up = normal_values(seeds[11], (EXPERTS, D, FF), D ** -0.5, 0.125, ((0, 64), (2, 4)))
    w_down = normal_values(seeds[12], (EXPERTS, FF, D), FF ** -0.5, 0.1875, ((0, 64), (1, 4)))
    return dict(queries=queries, keys=keys, values=values, query_gain=query_gain, key_gain=key_gain, out_weight=out_weight, moe_tokens=moe_tokens, moe_gain=moe_gain, routes=routes, route_weight=route_weight, w_gate=w_gate, w_up=w_up, w_down=w_down)


EPS = 1e-06
THETA = 10000.0

def turn(normed, positions):
    quarter = normed.shape[-1] // 4
    inverse = THETA ** (-jnp.arange(quarter, dtype=jnp.float32) / quarter)
    grid_row = (positions // GRID_W).astype(jnp.float32)
    grid_col = (positions % GRID_W).astype(jnp.float32)
    angles = jnp.stack([grid_row[:, None] * inverse, grid_col[:, None] * inverse], axis=1)
    cosine = jnp.cos(angles)[:, None, None]
    sine = jnp.sin(angles)[:, None, None]
    parts = normed.reshape(normed.shape[:-1] + (2, 2, quarter))
    first = parts[..., 0, :]
    second = parts[..., 1, :]
    turned = jnp.stack([first * cosine - second * sine, second * cosine + first * sine], axis=-2)
    return turned.reshape(normed.shape)

def prepare(data, positions, gain):
    heads = data.astype(jnp.float32).reshape(data.shape[0], data.shape[1], -1, HEAD_DIM)
    normed = heads * lax.rsqrt(lax.optimization_barrier(jnp.mean(heads * heads, axis=-1, keepdims=True)) + EPS) * gain
    return turn(normed, positions).astype(jnp.bfloat16)

def reference(queries, keys, values, query_gain, key_gain, out_weight, moe_tokens, moe_gain, routes, route_weight, w_gate, w_up, w_down):
    positions = jnp.arange(LEN, dtype=jnp.int32)
    q_rot = prepare(queries, positions, query_gain)
    k_rot = prepare(keys, positions, key_gain)
    key_float = k_rot.astype(jnp.float32)
    value_float = values.reshape(LEN, SEQS, KV_HEADS, HEAD_DIM).astype(jnp.float32)
    groups = HEADS // KV_HEADS
    block = math.gcd(LEN, 64)
    query_blocks = q_rot.reshape(LEN // block, block, SEQS, KV_HEADS, groups, HEAD_DIM)

    def attend(query_block):
        scores = jnp.einsum('bskgd,lskd->skgbl', query_block.astype(jnp.float32), key_float) * HEAD_DIM ** (-0.5)
        largest = lax.optimization_barrier(jnp.max(scores, axis=-1, keepdims=True))
        expo = jnp.exp(scores - largest)
        total = lax.optimization_barrier(jnp.sum(expo, axis=-1))
        probs = lax.optimization_barrier(expo.astype(jnp.bfloat16)).astype(jnp.float32)
        summed = jnp.einsum('skgbl,lskd->skgbd', probs, value_float) / total[..., None]
        return jnp.transpose(summed, (3, 0, 1, 2, 4)).astype(jnp.bfloat16)
    mixed = lax.map(attend, query_blocks).reshape(LEN * SEQS, HEADS * HEAD_DIM)
    width = HEADS * HEAD_DIM // N_TP
    accum = jnp.zeros((LEN * SEQS, D), jnp.float32)
    for index in range(N_TP):
        part = jnp.dot(mixed[:, index * width:(index + 1) * width], out_weight[index * width:(index + 1) * width], preferred_element_type=jnp.float32)
        accum = accum + lax.optimization_barrier(part.astype(jnp.bfloat16)).astype(jnp.float32)
    attended = accum.astype(jnp.bfloat16).reshape(LEN, SEQS, D)
    token_float = moe_tokens.astype(jnp.float32)
    normed = (token_float * lax.rsqrt(lax.optimization_barrier(jnp.mean(token_float * token_float, axis=-1, keepdims=True)) + EPS) * moe_gain).astype(jnp.bfloat16)
    most = N_EP * N_TP * CAP
    unit_width = FF // N_TP

    def expert(carry, item):
        index, gate_weight, up_weight, down_weight = item
        chosen = routes == index
        weight = lax.optimization_barrier(jnp.sum(jnp.where(chosen, route_weight, 0.0), axis=1))
        live = jnp.any(chosen, axis=1)
        rows = jnp.nonzero(live, size=most, fill_value=0)[0].astype(jnp.int32)
        count = jnp.sum(live.astype(jnp.int32))
        valid = (jnp.arange(most, dtype=jnp.int32) < count).astype(jnp.float32)
        picked = normed[rows]
        gate = jnp.dot(picked, gate_weight, preferred_element_type=jnp.float32)
        up = jnp.dot(picked, up_weight, preferred_element_type=jnp.float32)
        hidden = (jax.nn.silu(gate) * up).astype(jnp.bfloat16)
        out = jnp.zeros((most, D), jnp.float32)
        for block_index in range(N_TP):
            part = jnp.dot(hidden[:, block_index * unit_width:(block_index + 1) * unit_width], down_weight[block_index * unit_width:(block_index + 1) * unit_width], preferred_element_type=jnp.float32)
            out = out + lax.optimization_barrier(part.astype(jnp.bfloat16)).astype(jnp.float32)
        expert_out = lax.optimization_barrier(out.astype(jnp.bfloat16)).astype(jnp.float32)
        contrib = expert_out * (weight[rows] * valid)[:, None]
        return (carry.at[rows].add(contrib), None)
    routed, _ = lax.scan(expert, jnp.zeros((TOKENS, D), jnp.float32), (jnp.arange(EXPERTS, dtype=jnp.int32), w_gate, w_up, w_down))
    return (attended, routed.astype(jnp.bfloat16))
```

```python
import functools

import jax
import jax.numpy as jnp
from jax import lax
from jax.experimental import pallas as pl
from jax.experimental.pallas import tpu as pltpu
from jax.sharding import PartitionSpec as P

HEAD_DIM = 64
GRID_W = 64
EPS = 1e-06
THETA = 10000.0
CAP = 6
SLOT = 8
PACK = 1536
TAIL = 512
PLANE = 8
PLANES = 8
BLOCK = 256
QW = 1024
CHUNK = 2
LOG2E = 1.4426950408889634
MESH = pl.DeviceIdType.MESH
BF16 = jnp.bfloat16
F32 = jnp.float32


def rcopy(src, dst, send_sem, recv_sem, dev):
    return pltpu.make_async_remote_copy(
        src_ref=src,
        dst_ref=dst,
        send_sem=send_sem,
        recv_sem=recv_sem,
        device_id=dev,
        device_id_type=MESH,
    )


def wait_for(ref, sem):
    pltpu.make_async_copy(ref, ref, sem).wait()


def near_first(i):
    return (1 - 2 * lax.rem(i + 1, 2)) * ((i + 1) // 2)


def attend(group, tile, q2, kvbuf, s_ref, m_ref, acc_ref):
    scale = LOG2E * HEAD_DIM**-0.5
    cols = pl.ds(pl.multiple_of(tile * QW, QW), QW)
    pieces = PLANE // CHUNK
    m_old = m_ref[tile]
    for h in range(2):
        q = q2[h, :, cols]
        for p in range(pieces):
            k = kvbuf[pl.ds(group * PLANE + p * CHUNK, CHUNK), 0:128, :].reshape(CHUNK * 128, 128)
            s_ref[h, p] = jnp.dot(k, q, preferred_element_type=F32)
    best = m_old
    for h in range(2):
        for p in range(pieces):
            part = s_ref[h, p].reshape(CHUNK * 16, 8, QW)
            best = jnp.maximum(best, jnp.max(part, axis=0))
    top = jnp.max(best, axis=0, keepdims=True)
    m_new = jnp.broadcast_to(top, (8, QW))
    factor = jnp.exp2((m_old - m_new) * scale)
    shift = top * scale
    m_ref[tile] = m_new
    acc = acc_ref[tile] * jnp.broadcast_to(factor[0:1], (acc_ref.shape[1], QW))
    ones = jnp.ones((16, CHUNK * 128), BF16)
    for h in range(2):
        for p in range(pieces):
            probs = jnp.exp2(s_ref[h, p] * scale - shift).astype(BF16)
            v = jnp.concatenate(
                [
                    kvbuf[group * PLANE + p * CHUNK + b, 128 + 64 * h : 192 + 64 * h, :]
                    for b in range(CHUNK)
                ],
                axis=1,
            )
            acc = acc + jnp.dot(
                jnp.concatenate([v, ones], axis=0), probs, preferred_element_type=F32
            )
    acc_ref[tile] = acc


def kernel(
    send,
    kvp,
    qt,
    wg,
    wu,
    wd,
    wo,
    unpack,
    pack,
    ret,
    out_parts,
    recv,
    recv2,
    xbuf,
    wgb,
    wub,
    wdb,
    ybuf,
    part,
    rs,
    ret_send,
    kvbuf,
    qbuf,
    q2,
    s_ref,
    m_ref,
    acc_ref,
    obuf,
    sem_local,
    sem_send,
    sem_w,
    sem_d,
    sem_f,
    sem_rs,
    sem_ret,
    sem_x,
    sem_up,
    sem_down,
    sem_q,
    sem_o,
):
    me = lax.axis_index("ep")
    y = lax.axis_index("tp")
    z = me // PLANE
    inner = lax.rem(me, PLANE)
    core = lax.rem(me, 2)
    base = z * PLANE
    y_w = y + 1 - 2 * lax.rem(y, 2)
    y_t = 3 - y
    tiles = qbuf.shape[0] * qbuf.shape[2] // QW

    other = me + 1 - 2 * core
    q_copy = rcopy(qt.at[1 - core], qbuf.at[core], sem_send.at[0], sem_q, (other, y))
    q_copy.start()
    q_local = pltpu.make_async_copy(qt.at[core], qbuf.at[core], sem_local.at[0])

    def plane_peer(j):
        return lax.rem(inner + j, PLANE)

    def x_send(j, _):
        peer = plane_peer(j)
        rcopy(
            kvp.at[lax.rem(peer, 2)],
            kvbuf.at[me],
            sem_send.at[1],
            sem_x.at[inner],
            (base + peer, y),
        ).start()
        return 0

    lax.fori_loop(1, PLANE, x_send, 0)
    kv_local = pltpu.make_async_copy(kvp.at[core], kvbuf.at[me], sem_local.at[1])
    kv_local.start()

    w_copies = []
    for i, (src, dst) in enumerate(((wg, wgb), (wu, wub), (wd, wdb))):
        w_copy = rcopy(src, dst.at[1], sem_send.at[2 + i], sem_w.at[i], (me, y_w))
        w_copy.start()
        w_copies.append(w_copy)
    w_local = []
    for i, (src, dst) in enumerate(((wg, wgb), (wu, wub), (wd, wdb))):
        local = pltpu.make_async_copy(src, dst.at[0], sem_local.at[2 + i])
        local.start()
        w_local.append(local)

    def plane_at(i, sign):
        return lax.rem(z + sign * near_first(i) + 2 * PLANES, PLANES)

    def d_send(t, _):
        to = plane_at(t // PLANE, 1) * PLANE + lax.rem(t + inner, PLANE)

        @pl.when(to != me)
        def _():
            rcopy(send.at[to], recv.at[me], sem_send.at[5], sem_d.at[me], (to, y)).start()

        return 0

    lax.fori_loop(0, PLANES * PLANE, d_send, 0)
    d_local = pltpu.make_async_copy(send.at[me], recv.at[me], sem_local.at[5])
    d_local.start()

    q_local.start()
    m_ref[...] = jnp.full(m_ref.shape, -1e30, F32)
    acc_ref[...] = jnp.zeros(acc_ref.shape, F32)

    kv_local.wait()

    def x_wait(j, _):
        peer = plane_peer(j)
        wait_for(kvbuf.at[base + peer], sem_x.at[peer])
        return 0

    lax.fori_loop(1, PLANE, x_wait, 0)
    up = lax.rem(z + 1, PLANES) * PLANE + inner
    down = lax.rem(z + PLANES - 1, PLANES) * PLANE + inner

    def group_of(shift):
        return lax.rem(z + shift + 2 * PLANES, PLANES)

    def group_ref(group):
        return kvbuf.at[pl.ds(pl.multiple_of(group * PLANE, PLANE), PLANE)]

    def ring_up(step):
        g = group_ref(group_of(1 - step))
        rcopy(g, g, sem_send.at[6], sem_up.at[step - 1], (up, y)).start()

    def ring_down(step):
        g = group_ref(group_of(step - 1))
        rcopy(g, g, sem_send.at[7], sem_down.at[step - 1], (down, y)).start()

    def ring_wait_up(step):
        wait_for(group_ref(group_of(-step)), sem_up.at[step - 1])

    def ring_wait_down(step):
        wait_for(group_ref(group_of(step)), sem_down.at[step - 1])

    ring_up(1)
    ring_down(1)

    q_local.wait()
    q_copy.wait_recv()
    zeros = jnp.zeros((64, qbuf.shape[2]), BF16)
    for s in range(2):
        cols = slice(s * qbuf.shape[2], (s + 1) * qbuf.shape[2])
        q2[0, 0:64, cols] = qbuf[s]
        q2[0, 64:128, cols] = zeros
        q2[1, 0:64, cols] = zeros
        q2[1, 64:128, cols] = qbuf[s]

    def attend_groups(first, last):
        def body(i, _):
            n = first + i // tiles
            group = lax.rem(z - near_first(n) + 2 * PLANES, PLANES)
            attend(group, lax.rem(i, tiles), q2, kvbuf, s_ref, m_ref, acc_ref)
            return 0

        lax.fori_loop(0, (last - first) * tiles, body, 0)

    attend_groups(0, 1)

    def open_rows(src, plane, row0):
        rows = src[pl.ds(pl.multiple_of(plane * PLANE, PLANE), PLANE)].reshape(PLANE * SLOT, PACK)
        at = pl.ds(pl.multiple_of(row0 + plane * PLANE * CAP, 16), PLANE * CAP)
        main = jnp.dot(unpack[0], rows, preferred_element_type=F32)
        xbuf[at, 0:PACK] = main.astype(BF16)
        tail = jnp.dot(unpack[1], rows[:, 0:TAIL], preferred_element_type=F32)
        for k in range(1, 3):
            tail = tail + jnp.dot(
                unpack[1 + k], rows[:, k * TAIL : (k + 1) * TAIL], preferred_element_type=F32
            )
        xbuf[at, PACK : PACK + TAIL] = tail.astype(BF16)

    d_local.wait()

    def plane_ref(ref, plane):
        return ref.at[pl.ds(pl.multiple_of(plane * PLANE, PLANE), PLANE)]

    def arrive(i, _):
        plane = plane_at(i, -1)

        def one(j, _):
            src = plane * PLANE + j

            @pl.when(src != me)
            def _():
                wait_for(recv.at[src], sem_d.at[src])

            return 0

        lax.fori_loop(0, PLANE, one, 0)
        rcopy(
            plane_ref(recv, plane),
            plane_ref(recv2, plane),
            sem_send.at[8],
            sem_f.at[plane],
            (me, y_t),
        ).start()
        open_rows(recv, plane, 0)
        return 0

    lax.fori_loop(0, PLANES, arrive, 0)

    rows_own = PLANES * PLANE * CAP

    def arrive2(i, _):
        plane = lax.rem(z - near_first(i) + 2 * PLANES, PLANES)
        wait_for(plane_ref(recv2, plane), sem_f.at[plane])
        open_rows(recv2, plane, rows_own)
        return 0

    lax.fori_loop(0, PLANES, arrive2, 0)

    def ffn(blk, n):
        at = pl.ds(pl.multiple_of(n * 192, 16), 192)
        x = xbuf[at]
        gate = jnp.dot(x, wgb[blk], preferred_element_type=F32)
        lift = jnp.dot(x, wub[blk], preferred_element_type=F32)
        hidden = (jax.nn.silu(gate) * lift).astype(BF16)
        ybuf[blk, at, :] = jnp.dot(hidden, wdb[blk], preferred_element_type=F32).astype(BF16)

    for local in w_local:
        local.wait()

    def ffn_own(n, _):
        ffn(0, n)
        return 0

    lax.fori_loop(0, 4, ffn_own, 0)

    ring_wait_up(1)
    ring_wait_down(1)
    ring_up(2)
    ring_down(2)

    for w_copy in w_copies:
        w_copy.wait_recv()

    def share(n, _):
        ffn(1, 2 + n)

        def piece(j, _):
            plane = n * 4 + j
            at = pl.ds(pl.multiple_of(rows_own + plane * 48, 16), 48)
            both = ybuf[0, at, :].astype(F32) + ybuf[1, at, :].astype(F32)
            part[plane] = both.astype(BF16)
            return 0

        lax.fori_loop(0, 4, piece, 0)
        four = pl.ds(pl.multiple_of(n * 4, 4), 4)
        rcopy(part.at[four], rs.at[four], sem_send.at[9], sem_rs.at[n], (me, y_t)).start()
        return 0

    lax.fori_loop(0, 2, share, 0)

    def ffn_rest(n, _):
        ffn(1, n)
        return 0

    lax.fori_loop(0, 2, ffn_rest, 0)

    attend_groups(1, 3)
    ring_wait_up(2)
    ring_wait_down(2)
    ring_up(3)
    ring_down(3)

    def give_back(n, _):
        four = pl.ds(pl.multiple_of(n * 4, 4), 4)
        wait_for(rs.at[four], sem_rs.at[n])

        def one(i, _):
            plane = n * 4 + i
            at = pl.ds(pl.multiple_of(plane * 48, 16), 48)
            total = (
                ybuf[0, at, :].astype(F32) + ybuf[1, at, :].astype(F32) + rs[plane].astype(F32)
            ).astype(BF16)
            last = total[:, PACK : PACK + TAIL]
            for k in range(3):
                packed = jnp.dot(
                    pack[0], total[:, k * TAIL : (k + 1) * TAIL], preferred_element_type=F32
                ) + jnp.dot(pack[1 + k], last, preferred_element_type=F32)
                ret_send[
                    pl.ds(pl.multiple_of(plane * PLANE, PLANE), PLANE),
                    :,
                    k * TAIL : (k + 1) * TAIL,
                ] = packed.astype(BF16).reshape(PLANE, SLOT, TAIL)
            return 0

        lax.fori_loop(0, 4, one, 0)

        def out(j, _):
            to = n * 32 + lax.rem(j + inner, 32)

            @pl.when(to != me)
            def _():
                rcopy(
                    ret_send.at[to], ret.at[me], sem_send.at[10], sem_ret.at[me], (to, y)
                ).start()

            @pl.when(to == me)
            def _():
                pltpu.make_async_copy(ret_send.at[to], ret.at[me], sem_local.at[6]).start()

            return 0

        lax.fori_loop(0, 32, out, 0)
        return 0

    lax.fori_loop(0, 2, give_back, 0)

    attend_groups(3, 5)
    ring_wait_up(3)
    ring_wait_down(3)
    ring_up(4)
    attend_groups(5, 7)
    ring_wait_up(4)
    attend_groups(7, 8)

    def project(s, _):
        acc = acc_ref[s]
        mixed = (acc[0:64] / acc[64:65]).astype(BF16).astype(F32)
        heads = jnp.concatenate(
            [mixed[:, h * BLOCK : (h + 1) * BLOCK].T for h in range(QW // BLOCK)], axis=1
        ).astype(BF16)
        obuf[s] = jnp.dot(heads, wo[...], preferred_element_type=F32).astype(BF16)
        return 0

    lax.fori_loop(0, 2, project, 0)

    def o_send(j, _):
        to_y = lax.rem(y + j // 2, 4)
        to_core = lax.rem(core + j, 2)
        src = obuf.at[to_core, pl.ds(pl.multiple_of(to_y * 64, 64), 64)]
        rcopy(
            src,
            out_parts.at[core, y],
            sem_send.at[11],
            sem_o.at[core * 4 + y],
            (me - core + to_core, to_y),
        ).start()
        return 0

    lax.fori_loop(1, 8, o_send, 0)
    o_local = pltpu.make_async_copy(
        obuf.at[core, pl.ds(pl.multiple_of(y * 64, 64), 64)], out_parts.at[core, y], sem_local.at[7]
    )
    o_local.start()

    def o_wait(j, _):
        from_y = lax.rem(y + j // 2, 4)
        from_core = lax.rem(core + j, 2)
        wait_for(out_parts.at[from_core, from_y], sem_o.at[from_core * 4 + from_y])
        return 0

    lax.fori_loop(1, 8, o_wait, 0)
    o_local.wait()

    def ret_wait(j, _):
        src = lax.rem(me + j, 64)
        wait_for(ret.at[src], sem_ret.at[src])
        return 0

    lax.fori_loop(1, 64, ret_wait, 0)
    wait_for(ret.at[me], sem_local.at[6])

    q_copy.wait_send()
    wait_for(kvbuf.at[pl.ds(0, 7)], sem_send.at[1])
    for w_copy in w_copies:
        w_copy.wait_send()
    wait_for(recv.at[pl.ds(0, 63)], sem_send.at[5])
    wait_for(kvbuf.at[pl.ds(0, 32)], sem_send.at[6])
    wait_for(kvbuf.at[pl.ds(0, 24)], sem_send.at[7])
    wait_for(recv, sem_send.at[8])
    wait_for(part, sem_send.at[9])
    wait_for(recv.at[pl.ds(0, 63)], sem_send.at[10])
    wait_for(xbuf.at[pl.ds(0, 448)], sem_send.at[11])


def call_kernel(send, kvp, qt, wg, wu, wd, wo, unpack, pack):
    any_space = pl.BlockSpec(memory_space=pl.ANY)
    vmem = pl.BlockSpec(memory_space=pltpu.VMEM)
    dma = pltpu.SemaphoreType.DMA
    n_tiles = 2 * qt.shape[2] // QW
    return pl.pallas_call(
        kernel,
        out_shape=(
            jax.ShapeDtypeStruct(send.shape, BF16),
            jax.ShapeDtypeStruct((2, 4, 64, wo.shape[1]), BF16),
        ),
        in_specs=[any_space] * 6 + [vmem] * 3,
        out_specs=(any_space, any_space),
        scratch_shapes=[
            pltpu.VMEM(send.shape, BF16),
            pltpu.VMEM(send.shape, BF16),
            pltpu.VMEM((768, 2048), BF16),
            pltpu.VMEM((2,) + wg.shape, BF16),
            pltpu.VMEM((2,) + wu.shape, BF16),
            pltpu.VMEM((2,) + wd.shape, BF16),
            pltpu.VMEM((2, 768, 2048), BF16),
            pltpu.VMEM((8, 48, 2048), BF16),
            pltpu.VMEM((8, 48, 2048), BF16),
            pltpu.VMEM(send.shape, BF16),
            pltpu.VMEM((64, 256, 128), BF16),
            pltpu.VMEM((2,) + qt.shape[1:], BF16),
            pltpu.VMEM((2, 128, 2 * qt.shape[2]), BF16),
            pltpu.VMEM((2, PLANE // CHUNK, CHUNK * 128, QW), F32),
            pltpu.VMEM((n_tiles, 8, QW), F32),
            pltpu.VMEM((n_tiles, 80, QW), F32),
            pltpu.VMEM((2, BLOCK, wo.shape[1]), BF16),
            dma((8,)),
            dma((12,)),
            dma((3,)),
            dma((64,)),
            dma((8,)),
            dma((2,)),
            dma((64,)),
            dma((8,)),
            dma((4,)),
            dma((3,)),
            dma(()),
            dma((8,)),
        ],
        compiler_params=pltpu.CompilerParams(has_side_effects=True, vmem_limit_bytes=60 * 2**20),
        name="mega",
    )(send, kvp, qt, wg, wu, wd, wo, unpack, pack)


def turn(normed, positions):
    quarter = normed.shape[-1] // 4
    inverse = THETA ** (-jnp.arange(quarter, dtype=F32) / quarter)
    grid_row = (positions // GRID_W).astype(F32)
    grid_col = (positions % GRID_W).astype(F32)
    angles = jnp.stack([grid_row[:, None] * inverse, grid_col[:, None] * inverse], axis=1)
    cosine = jnp.cos(angles)[:, None, None]
    sine = jnp.sin(angles)[:, None, None]
    parts = normed.reshape(normed.shape[:-1] + (2, 2, quarter))
    first = parts[..., 0, :]
    second = parts[..., 1, :]
    turned = jnp.stack([first * cosine - second * sine, second * cosine + first * sine], axis=-2)
    return turned.reshape(normed.shape)


def prepare(data, positions, gain):
    heads = data.astype(F32).reshape(data.shape[0], data.shape[1], -1, HEAD_DIM)
    normed = heads * lax.rsqrt(jnp.mean(heads * heads, axis=-1, keepdims=True) + EPS) * gain
    return turn(normed, positions).astype(BF16)


def one_hot_packing():
    row = jnp.arange(PLANE * CAP, dtype=jnp.int32)[:, None]
    col = jnp.arange(PLANE * SLOT, dtype=jnp.int32)[None, :]
    same = row // CAP == col // SLOT
    r, s = row % CAP, col % SLOT
    picks = [same & (r == s)] + [same & (s == CAP + r // 3) & (r % 3 == k) for k in range(3)]
    unpack = jnp.stack(picks).astype(BF16)
    return unpack, jnp.swapaxes(unpack, 1, 2)


def per_device(
    queries,
    keys,
    values,
    query_gain,
    key_gain,
    out_weight,
    moe_tokens,
    moe_gain,
    routes,
    route_weight,
    w_gate,
    w_up,
    w_down,
):
    pos_count, seq_count = queries.shape[0], queries.shape[1]
    positions = lax.axis_index("ep") * pos_count + jnp.arange(pos_count, dtype=jnp.int32)
    q_rot = prepare(queries, positions, query_gain)
    k_rot = prepare(keys, positions, key_gain)[:, :, 0]
    qt = jnp.transpose(q_rot, (1, 3, 2, 0)).reshape(seq_count, HEAD_DIM, -1)
    half = pos_count // 2
    k_two = jnp.concatenate([k_rot[:half], k_rot[half:]], axis=-1)
    k_two = jnp.transpose(k_two, (1, 0, 2))
    v_two = jnp.transpose(values.reshape(2, half, seq_count, HEAD_DIM), (2, 0, 3, 1))
    kvp = jnp.concatenate([k_two, v_two.reshape(seq_count, 2 * HEAD_DIM, half)], axis=1)

    tok_count, top_count = routes.shape
    experts = lax.axis_size("ep")
    token_float = moe_tokens.astype(F32)
    normed = (
        token_float
        * lax.rsqrt(jnp.mean(token_float * token_float, axis=-1, keepdims=True) + EPS)
        * moe_gain
    ).astype(BF16)
    hits = (routes[:, :, None] == jnp.arange(experts, dtype=jnp.int32)[None, None, :]).astype(BF16)
    pair_count = tok_count * top_count
    flat_hits = hits.reshape(pair_count, experts)
    pair_index = jnp.arange(pair_count, dtype=jnp.int32)
    earlier = (pair_index[:, None] > pair_index[None, :]).astype(BF16)
    before = jnp.dot(earlier, flat_hits, preferred_element_type=F32)
    rank = jnp.sum(before * flat_hits.astype(F32), axis=-1).astype(jnp.int32)
    rank = rank.reshape(tok_count, top_count)
    main = routes * SLOT + rank
    rest = routes * SLOT + CAP + rank // 3
    third = rank % 3
    table = jnp.arange(experts * SLOT, dtype=jnp.int32)

    def spread(slot, keep):
        hit = (slot[None, :, :] == table[:, None, None]) & keep[None]
        return jnp.any(hit, axis=2).astype(BF16)

    first = spread(main, third >= 0)
    columns = []
    for k in range(3):
        lhs = jnp.concatenate([first, spread(rest, third == k)], axis=1)
        rhs = jnp.concatenate(
            [normed[:, k * TAIL : (k + 1) * TAIL], normed[:, PACK : PACK + TAIL]], axis=0
        )
        columns.append(jnp.dot(lhs, rhs, preferred_element_type=F32).astype(BF16))
    send = jnp.concatenate(columns, axis=1).reshape(experts, SLOT, PACK)

    unpack, pack = one_hot_packing()
    ret, out_parts = call_kernel(
        send, kvp, qt, w_gate[0], w_up[0], w_down[0], out_weight, unpack, pack
    )

    attended = jnp.transpose(out_parts.astype(F32).sum(axis=1), (1, 0, 2)).astype(BF16)

    rows = ret.reshape(experts * SLOT, PACK)
    combined = jnp.zeros((tok_count, PACK + TAIL), F32)
    for choice in range(top_count):
        pick = slice(choice, choice + 1)
        lead = (main[:, pick] == table[None, :]).astype(BF16)
        picked = jnp.dot(lead, rows, preferred_element_type=F32)
        tail = jnp.zeros((tok_count, TAIL), F32)
        for k in range(3):
            follow = ((rest[:, pick] == table[None, :]) & (third[:, pick] == k)).astype(BF16)
            tail = tail + jnp.dot(
                follow, rows[:, k * TAIL : (k + 1) * TAIL], preferred_element_type=F32
            )
        picked = jnp.concatenate([picked, tail], axis=1)
        combined = combined + picked * route_weight[:, pick]
    return (attended, combined.astype(BF16))


def solution(mesh):
    in_specs = (
        P("ep", None, "tp"),
        P("ep", None, "tp"),
        P("ep", None, "tp"),
        P(),
        P(),
        P("tp", None),
        P(("ep", "tp"), None),
        P(),
        P(("ep", "tp"), None),
        P(("ep", "tp"), None),
        P("ep", None, "tp"),
        P("ep", None, "tp"),
        P("ep", "tp", None),
    )
    out_specs = (P(("ep", "tp"), None, None), P(("ep", "tp"), None))
    return jax.shard_map(
        per_device, mesh=mesh, in_specs=in_specs, out_specs=out_specs, check_vma=False
    )
```
